32 devices in a mesh: rep: 2 (over x), fs: 4 (over z), tp: 4 (over y, core).
Axes of the slice: x: 2, y: 2, z: 4, core: 2. Of those that a mesh axis runs over, the one named last changes fastest.
Arguments:
- tokens: bfloat16 [8192, 2048], P(('rep', 'fs'), 'tp'), may hold values from -6 to 6
- mix_in_gain: bfloat16 [2048], replicated, may hold values from 0.099609375 to 1.8984375
- bgate_weight: bfloat16 [2048, 2048], P('fs', 'tp'), may hold values from -0.125 to 0.125
- cgate_weight: bfloat16 [2048, 2048], P('fs', 'tp'), may hold values from -0.125 to 0.125
- value_weight: bfloat16 [2048, 2048], P('fs', 'tp'), may hold values from -0.125 to 0.125
- conv_taps: bfloat16 [3, 2048], replicated, may hold values from -3 to 3
- out_weight: bfloat16 [2048, 2048], P('tp', 'fs'), may hold values from -0.41984465 to 0.41984465
- mix_out_gain: bfloat16 [2048], replicated, may hold values from 0.099609375 to 1.8984375
- ffn_in_gain: bfloat16 [2048], replicated, may hold values from 0.099609375 to 1.8984375
- up_weight: bfloat16 [2048, 8192], P('fs', 'tp'), may hold values from -0.125 to 0.125
- down_weight: bfloat16 [8192, 2048], P('tp', 'fs'), may hold values from -0.20992233 to 0.20992233
- ffn_out_gain: bfloat16 [2048], replicated, may hold values from 0.099609375 to 1.8984375
Outputs:
- result: bfloat16 [8192, 2048], P(('rep', 'fs'), 'tp')
The draws below stay inside these ranges and needn't reach their ends.
All inputs are finite; a program needn't handle non-finite values.
Results may differ from the reference program's by a relative error of at most 0.02.
Values may be sent and summed in bfloat16 or wider, within the bound.
A program may use at most 128 MiB of HBM per device.

```python
import jax
import jax.numpy as jnp
from jax import lax

D = 2048
CW = 2048
FF = 8192
LEN = 256
TOKENS = 8192
N_TP = 4


def rising_matrix(base, rows, cols, top):
    ramp = top ** (jnp.arange(cols, dtype=jnp.float32) / cols)
    return (base * ramp[None, :] * rows ** (-0.5)).astype(jnp.bfloat16)


def draw_out_weight(key, part):
    own_key = jax.random.fold_in(key, 11)
    base = jnp.clip(jax.random.normal(own_key, (CW, D), jnp.float32), -6.0, 6.0)
    return rising_matrix(base, CW, D, 3.0)


def draw_down_weight(key, part):
    own_key = jax.random.fold_in(key, 23)
    base = jnp.clip(jax.random.normal(own_key, (FF, D), jnp.float32), -6.0, 6.0)
    return rising_matrix(base, FF, D, 3.0)


def shard_levels(key, extent, split, least, top_value):
    def one(position, blocks):
        steps = jax.random.uniform(jax.random.fold_in(jax.random.fold_in(key, 6), position), (blocks,), jnp.float32, least / len(split), top_value / len(split))
        return jnp.repeat(jnp.exp(steps), extent[position] // blocks).reshape((-1,) + (1,) * (len(extent) - position - 1))

    level = one(*split[0])
    for cut in split[1:]:
        level = level * one(*cut)
    return level


def centred(key, extent, spread, reach, split=(), kind=jnp.bfloat16):
    level = shard_levels(key, extent, split, -0.22, 0.18) if split else 1.0
    drawn = jax.random.normal(key, extent, jnp.float32) * spread * level
    return jnp.minimum(jnp.maximum(drawn, -reach), reach).astype(kind)


def setup_inputs(seed: int = 0) -> dict:
    arg_keys = jax.random.split(jax.random.key(seed), 13)
    return {
        "tokens": centred(arg_keys[0], (TOKENS, D), 1.0, 6.0, ((0, 8), (1, 4))),
        "mix_in_gain": jnp.clip(1.0 + 0.18 * jax.random.normal(arg_keys[1], (D,), jnp.float32), 0.099609375, 1.8984375).astype(jnp.bfloat16),
        "bgate_weight": centred(arg_keys[2], (D, CW), D ** -0.5, 0.125, ((0, 4), (1, 4))),
        "cgate_weight": centred(arg_keys[3], (D, CW), D ** -0.5, 0.125, ((0, 4), (1, 4))),
        "value_weight": centred(arg_keys[4], (D, CW), D ** -0.5, 0.125, ((0, 4), (1, 4))),
        "conv_taps": centred(arg_keys[5], (3, CW), 0.6, 3.0),
        "out_weight": draw_out_weight(jax.random.fold_in(arg_keys[12], 71), 0),
        "mix_out_gain": jnp.clip(1.0 + 0.18 * jax.random.normal(arg_keys[7], (D,), jnp.float32), 0.099609375, 1.8984375).astype(jnp.bfloat16),
        "ffn_in_gain": jnp.clip(1.0 + 0.18 * jax.random.normal(arg_keys[8], (D,), jnp.float32), 0.099609375, 1.8984375).astype(jnp.bfloat16),
        "up_weight": centred(arg_keys[9], (D, FF), D ** -0.5, 0.125, ((0, 4), (1, 4))),
        "down_weight": draw_down_weight(jax.random.fold_in(arg_keys[12], 71), 0),
        "ffn_out_gain": jnp.clip(1.0 + 0.18 * jax.random.normal(arg_keys[11], (D,), jnp.float32), 0.099609375, 1.8984375).astype(jnp.bfloat16),
    }


epsilon = 1e-06

def normalize(rows, gain):
    rows = rows.astype(jnp.float32)
    factor = lax.rsqrt(lax.optimization_barrier(jnp.mean(rows * rows, axis=-1, keepdims=True)) + epsilon)
    return rows * factor * gain.astype(jnp.float32)

def block_sum(left, right, blocks):
    width = left.shape[1] // blocks

    def step(total, index):
        start = (index * width).astype(jnp.int32)
        piece_left = lax.dynamic_slice_in_dim(left, start, width, 1)
        piece_right = lax.dynamic_slice_in_dim(right, start, width, 0)
        partial_term = jnp.dot(piece_left, piece_right, preferred_element_type=jnp.float32).astype(jnp.bfloat16)
        return (total + partial_term.astype(jnp.float32), None)
    start_total = jnp.zeros((left.shape[0], right.shape[1]), jnp.float32)
    total, _ = lax.scan(step, start_total, jnp.arange(blocks, dtype=jnp.int32))
    return total

def convolve(inner, taps):
    seqs = inner.reshape(-1, LEN, inner.shape[1])
    padded = jnp.pad(seqs, ((0, 0), (1, 1), (0, 0)))
    weights = taps.astype(jnp.float32)
    out = weights[0] * padded[:, :-2] + weights[1] * padded[:, 1:-1] + weights[2] * padded[:, 2:]
    return out.reshape(inner.shape)

def reference(tokens, mix_in_gain, bgate_weight, cgate_weight, value_weight, conv_taps, out_weight, mix_out_gain, ffn_in_gain, up_weight, down_weight, ffn_out_gain):
    normed = normalize(tokens, mix_in_gain).astype(jnp.bfloat16)
    bgate = jnp.dot(normed, bgate_weight, preferred_element_type=jnp.float32).astype(jnp.bfloat16)
    cgate = jnp.dot(normed, cgate_weight, preferred_element_type=jnp.float32).astype(jnp.bfloat16)
    value = jnp.dot(normed, value_weight, preferred_element_type=jnp.float32).astype(jnp.bfloat16)
    inner = cgate.astype(jnp.float32) * value.astype(jnp.float32)
    gated = (bgate.astype(jnp.float32) * convolve(inner, conv_taps)).astype(jnp.bfloat16)
    mixed = block_sum(gated, out_weight, N_TP)
    resid = (tokens.astype(jnp.float32) + normalize(mixed, mix_out_gain)).astype(jnp.bfloat16)
    second = normalize(resid, ffn_in_gain).astype(jnp.bfloat16)
    lifted = jnp.dot(second, up_weight, preferred_element_type=jnp.float32)
    active = jnp.square(jnp.maximum(lifted, 0.0)).astype(jnp.bfloat16)
    ffn = block_sum(active, down_weight, N_TP)
    return (resid.astype(jnp.float32) + normalize(ffn, ffn_out_gain)).astype(jnp.bfloat16)
```

```python
import functools

import jax
import jax.numpy as jnp
from jax import lax
from jax.experimental import pallas as pl
from jax.experimental.pallas import tpu as pltpu
from jax.sharding import PartitionSpec as P

LEN = 256
LANES = 128
AHEAD = 3

epsilon = 1e-06
MESH = pl.DeviceIdType.MESH
F32 = jnp.float32
BF16 = jnp.bfloat16


def at(index, size):
    return pl.ds(pl.multiple_of(index * size, size), size)


def dot(left, right):
    return jnp.dot(left, right, preferred_element_type=F32)


def kernel(
    nfs, ntp, nu, nc, cw,
    tokens, gain1, wb, wc, wv, taps, wo, gain2, gain3, wu, wd, gain4,
    result,
    rows_w, out_w, down_w, tok, normed, part, rs, mix, active, energy,
    recv_z, recv_x, send_r, send_l, send_x, local_sem, tok_local,
    tok_send, tok_recv, rs_send, rs_recv, ag_send, ag_recv, ff_send, ff_recv, en_send, en_recv,
):
    rep, fs, tp = lax.axis_index("rep"), lax.axis_index("fs"), lax.axis_index("tp")
    count, own = tokens.shape
    width = own * ntp
    seqs = count // LEN
    krows = wb.shape[0]
    chan = wb.shape[1]
    ucol = wu.shape[1] // nu
    ocol = wo.shape[1]
    nk = 3 + 1 + nu + nc
    first_down = 4 + nu

    barrier = pltpu.get_barrier_semaphore()
    for step in (1, nfs - 1):
        pl.semaphore_signal(barrier, inc=1, device_id={"fs": lax.rem(fs + step, nfs)}, device_id_type=MESH)
    pl.semaphore_signal(barrier, inc=1, device_id={"rep": 1 - rep}, device_id_type=MESH)
    for step in range(1, ntp):
        pl.semaphore_signal(barrier, inc=1, device_id={"tp": lax.rem(tp + step, ntp)}, device_id_type=MESH)
    pl.semaphore_wait(barrier, 3 + ntp - 1)

    def region(k, s, half):
        if k < 3 or 4 <= k < first_down:
            index = k if k < 3 else k - 1
            if half is None:
                return rows_w.at[index, at(s, krows), :]
            return rows_w.at[index, at(s * 2 + half, krows // 2), :]
        if k == 3:
            r = slice(None) if half is None else at(half, wo.shape[0] // 2)
            return out_w.at[r, at(s, ocol)]
        r = slice(None) if half is None else at(half, wd.shape[0] // 2)
        return down_w.at[k - first_down, r, at(s, cw)]

    def source(k, half):
        if k < 3:
            ref, c = (wb, wc, wv)[k], slice(None)
        elif k == 3:
            ref, c = wo, slice(None)
        elif k < first_down:
            ref, c = wu, pl.ds((k - 4) * ucol, ucol)
        else:
            ref, c = wd, pl.ds((k - first_down) * cw, cw)
        r = slice(None) if half is None else at(half, ref.shape[0] // 2)
        return ref.at[r, c]

    def hop(k, s, src, sems, to):
        return pltpu.make_async_remote_copy(
            src, region(k, s, rep), sems.at[k, s], recv_z.at[k, s],
            device_id={"fs": to}, device_id_type=MESH)

    def right(k, s, src=None):
        return hop(k, s, region(k, s, rep) if src is None else src, send_r, lax.rem(fs + 1, nfs))

    def left(k, s, src=None):
        return hop(k, s, region(k, s, rep) if src is None else src, send_l, lax.rem(fs + nfs - 1, nfs))

    def across(k, s, half):
        return pltpu.make_async_remote_copy(
            region(k, s, half), region(k, s, half), send_x.at[k, s], recv_x.at[k, s],
            device_id={"rep": 1 - rep}, device_id_type=MESH)

    def send_own(k):
        @pl.when(fs < nfs - 1)
        def _():
            right(k, fs, source(k, rep)).start()

        @pl.when(fs > 0)
        def _():
            left(k, fs, source(k, rep)).start()

    def local(k):
        return pltpu.make_async_copy(source(k, None), region(k, fs, None), local_sem.at[k])

    def advance(k):
        if k + AHEAD < nk:
            send_own(k + AHEAD)

        def one(d, carry):
            @pl.when(fs - d >= 0)
            def _():
                s = fs - d
                right(k, s).wait_recv()

                @pl.when(fs < nfs - 1)
                def _():
                    right(k, s).start()

                across(k, s, rep).start()

            @pl.when(fs + d < nfs)
            def _():
                s = fs + d
                left(k, s).wait_recv()

                @pl.when(fs > 0)
                def _():
                    left(k, s).start()

                across(k, s, rep).start()

            return carry

        lax.fori_loop(1, nfs, one, 0)

    def complete(k):
        def one(s, carry):
            @pl.when(s != fs)
            def _():
                across(k, s, 1 - rep).wait_recv()

            return carry

        lax.fori_loop(0, nfs, one, 0)
        local(k).wait()

    def drain(k):
        def one(s, carry):
            @pl.when((s <= fs) & (fs < nfs - 1))
            def _():
                right(k, s).wait_send()

            @pl.when((s >= fs) & (fs > 0))
            def _():
                left(k, s).wait_send()

            @pl.when(s != fs)
            def _():
                across(k, s, rep).wait_send()

            return carry

        lax.fori_loop(0, nfs, one, 0)

    def group(t, src, dst, send, recv):
        return pltpu.make_async_remote_copy(
            src, dst, send, recv,
            device_id={"tp": lax.rem(tp + t, ntp)}, device_id_type=MESH)

    def tok_copy(t):
        mine = tok.at[:, at(tp, own)]
        return group(t, tokens, mine, tok_send.at[t - 1], tok_recv.at[t - 1])

    def rs_copy(t):
        to = lax.rem(tp + t, ntp)
        return group(t, part.at[:, at(to, own)], rs.at[t - 1], rs_send.at[t - 1], rs_recv.at[t - 1])

    def ag_copy(t):
        mine = mix.at[:, at(tp, own)]
        return group(t, mine, mine, ag_send.at[t - 1], ag_recv.at[t - 1])

    block = nfs * cw
    piece = block // ntp

    def ff_copy(t, c):
        to = lax.rem(tp + t, ntp)
        src = part.at[:, at(c * ntp + to, piece)]
        return group(t, src, rs.at[t - 1, :, pl.ds(c * piece, piece)], ff_send.at[t - 1, c], ff_recv.at[t - 1, c])

    def en_copy(t):
        return group(t, energy.at[0], energy.at[t], en_send.at[t - 1], en_recv.at[t - 1])

    def each_seq(fn):
        def one(i, carry):
            fn(at(i, LEN))
            return carry

        lax.fori_loop(0, seqs, one, 0)

    def factor(v):
        return lax.rsqrt(jnp.mean(v * v, axis=-1, keepdims=True) + epsilon)

    send_own(0)
    for t in range(1, ntp):
        tok_copy(t).start()
    own_tok = pltpu.make_async_copy(tokens, tok.at[:, at(tp, own)], tok_local)
    own_tok.start()
    for k in range(1, AHEAD):
        send_own(k)
    for k in range(nk):
        local(k).start()

    advance(0)
    advance(1)
    own_tok.wait()
    for t in range(1, ntp):
        tok_copy(t).wait_recv()

    def norm_tokens(r):
        v = tok[r, :].astype(F32)
        normed[r, :] = (v * factor(v) * gain1[...].astype(F32)).astype(BF16)

    each_seq(norm_tokens)
    advance(2)
    advance(3)
    for k in range(3):
        complete(k)

    own_taps = taps[:, at(tp, chan)].astype(F32)
    position = lax.broadcasted_iota(jnp.int32, (LEN, chan), 0)

    def mixer(r):
        rows = normed[r, :]
        inner = dot(rows, rows_w[1]).astype(BF16).astype(F32) * dot(rows, rows_w[2]).astype(BF16).astype(F32)
        before = jnp.where(position == 0, 0.0, pltpu.roll(inner, 1, 0))
        after = jnp.where(position == LEN - 1, 0.0, pltpu.roll(inner, LEN - 1, 0))
        conv = own_taps[0:1] * before + own_taps[1:2] * inner + own_taps[2:3] * after
        outer = dot(rows, rows_w[0]).astype(BF16).astype(F32)
        active[r, 0:chan] = (outer * conv).astype(BF16)

    each_seq(mixer)
    advance(4)
    complete(3)

    def project(r):
        part[r, :] = dot(active[r, 0:chan], out_w[...]).astype(BF16)

    each_seq(project)
    for t in range(1, ntp):
        rs_copy(t).start()
    done = 5
    for k in range(done, min(first_down, nk)):
        advance(k)
    for t in range(1, ntp):
        rs_copy(t).wait_recv()

    def add_mix(r):
        total = part[r, at(tp, own)].astype(F32)
        for t in range(1, ntp):
            total = total + rs[t - 1, r, :].astype(F32)
        mix[r, at(tp, own)] = total.astype(BF16)

    each_seq(add_mix)
    for t in range(1, ntp):
        ag_copy(t).start()
    early = max(nc - 2, 0)
    for c in range(early):
        advance(first_down + c)
    for k in range(4, first_down):
        complete(k)
    for t in range(1, ntp):
        ag_copy(t).wait_recv()

    def second(r):
        m = mix[r, :].astype(F32)
        res = (tok[r, :].astype(F32) + m * factor(m) * gain2[...].astype(F32)).astype(BF16)
        tok[r, :] = res
        res = res.astype(F32)
        rows = (res * factor(res) * gain3[...].astype(F32)).astype(BF16)
        for u in range(nu):
            lifted = jnp.maximum(dot(rows, rows_w[3 + u]), 0.0)
            active[r, pl.ds(u * ucol, ucol)] = (lifted * lifted).astype(BF16)

    for t in range(1, ntp):
        tok_copy(t).wait_send()
        rs_copy(t).wait_send()
    each_seq(second)

    for c in range(nc):
        if early <= c + 1 < nc:
            advance(first_down + c + 1)
        if c == 0 and early == 0:
            advance(first_down)
        complete(first_down + c)

        def down(r):
            part[r, pl.ds(c * block, block)] = dot(active[r, :], down_w[c]).astype(BF16)

        each_seq(down)
        for t in range(1, ntp):
            ff_copy(t, c).start()

    for k in range(nk):
        drain(k)
    for t in range(1, ntp):
        ag_copy(t).wait_send()
        for c in range(nc):
            ff_copy(t, c).wait_recv()

    def own_ffn(r):
        pieces = [part[r, at(c * ntp + tp, piece)] for c in range(nc)]
        total = (pieces[0] if nc == 1 else jnp.concatenate(pieces, axis=1)).astype(F32)
        for t in range(1, ntp):
            total = total + rs[t - 1, r, :].astype(F32)
        return total

    def measure(r):
        total = own_ffn(r)
        square = jnp.sum(total * total, axis=1, keepdims=True)
        flat = jnp.transpose(jnp.broadcast_to(square, (LEN, LANES)))
        energy[0, :, r] = flat[0:8, :]

    each_seq(measure)
    for t in range(1, ntp):
        en_copy(t).start()
    for t in range(1, ntp):
        en_copy(t).wait_recv()
    own_gain = gain4[:, at(tp, own)].astype(F32)

    def close(r):
        total = own_ffn(r)
        flat = energy[0, :, r]
        for t in range(1, ntp):
            flat = flat + energy[t, :, r]
        tall = jnp.transpose(jnp.concatenate([flat] * (LANES // 8), axis=0))
        scale = lax.rsqrt(tall[:, 0:1] / width + epsilon)
        result[r, :] = (tok[r, at(tp, own)].astype(F32) + total * scale * own_gain).astype(BF16)

    each_seq(close)
    for t in range(1, ntp):
        en_copy(t).wait_send()
        for c in range(nc):
            ff_copy(t, c).wait_send()


def solution(mesh):
    nfs, ntp = mesh.shape["fs"], mesh.shape["tp"]
    assert mesh.shape["rep"] == 2

    def body(tokens, gain1, wb, wc, wv, taps, wo, gain2, gain3, wu, wd, gain4):
        count, own = tokens.shape
        width, chan, hidden = own * ntp, wb.shape[1], wu.shape[1]
        ucol = chan
        nu = hidden // ucol
        cw = min(LANES, wd.shape[1])
        nc = wd.shape[1] // cw
        nk = 4 + nu + nc
        vm, anyw = pl.BlockSpec(memory_space=pltpu.VMEM), pl.BlockSpec(memory_space=pl.ANY)
        dma = pltpu.SemaphoreType.DMA
        peers = ntp - 1
        return pl.pallas_call(
            functools.partial(kernel, nfs, ntp, nu, nc, cw),
            out_shape=jax.ShapeDtypeStruct((count, own), BF16),
            in_specs=[anyw, vm, anyw, anyw, anyw, vm, anyw, vm, vm, anyw, anyw, vm],
            out_specs=vm,
            scratch_shapes=[
                pltpu.VMEM((3 + nu, width, chan), BF16),
                pltpu.VMEM((chan, width), BF16),
                pltpu.VMEM((nc, hidden, nfs * cw), BF16),
                pltpu.VMEM((count, width), BF16),
                pltpu.VMEM((count, width), BF16),
                pltpu.VMEM((count, width), BF16),
                pltpu.VMEM((peers, count, own), BF16),
                pltpu.VMEM((count, width), BF16),
                pltpu.VMEM((count, hidden), BF16),
                pltpu.VMEM((ntp, 8, count), F32),
                dma((nk, nfs)), dma((nk, nfs)), dma((nk, nfs)), dma((nk, nfs)), dma((nk, nfs)),
                dma((nk,)), dma,
                dma((peers,)), dma((peers,)), dma((peers,)), dma((peers,)),
                dma((peers,)), dma((peers,)), dma((peers, nc)), dma((peers, nc)),
                dma((peers,)), dma((peers,)),
            ],
            compiler_params=pltpu.CompilerParams(
                collective_id=0, has_side_effects=True, vmem_limit_bytes=64000000),
            name="layer",
        )(tokens, gain1[None], wb, wc, wv, taps, wo, gain2[None], gain3[None], wu, wd, gain4[None])

    placed = (
        P(("rep", "fs"), "tp"), P(), P("fs", "tp"), P("fs", "tp"), P("fs", "tp"), P(), P("tp", "fs"),
        P(), P(), P("fs", "tp"), P("tp", "fs"), P(),
    )
    return jax.shard_map(
        body, mesh=mesh, in_specs=placed, out_specs=P(("rep", "fs"), "tp"), check_vma=False
    )
```

```python
import functools

import jax
import jax.numpy as jnp
from jax import lax
from jax.experimental import pallas as pl
from jax.experimental.pallas import tpu as pltpu
from jax.sharding import PartitionSpec as P

LEN = 256
LANES = 128
AHEAD = 1

epsilon = 1e-06
MESH = pl.DeviceIdType.MESH
F32 = jnp.float32
BF16 = jnp.bfloat16


def at(index, size):
    return pl.ds(pl.multiple_of(index * size, size), size)


def dot(left, right):
    return jnp.dot(left, right, preferred_element_type=F32)


def kernel(
    nfs, ntp, nu, nc, cw,
    tokens, gain1, wb, wc, wv, taps, wo, gain2, gain3, wu, wd, gain4,
    result,
    rows_w, out_w, down_w, tok, normed, part, rs, mix, active, energy,
    recv_z, recv_x, send_r, send_l, send_x, local_sem, tok_local,
    tok_send, tok_recv, rs_send, rs_recv, ag_send, ag_recv, ff_send, ff_recv, en_send, en_recv,
):
    rep, fs, tp = lax.axis_index("rep"), lax.axis_index("fs"), lax.axis_index("tp")
    count, own = tokens.shape
    width = own * ntp
    seqs = count // LEN
    krows = wb.shape[0]
    chan = wb.shape[1]
    ucol = wu.shape[1] // nu
    ocol = wo.shape[1]
    nk = 3 + 1 + nu + nc
    first_down = 4 + nu

    barrier = pltpu.get_barrier_semaphore()
    for step in (1, nfs - 1):
        pl.semaphore_signal(barrier, inc=1, device_id={"fs": lax.rem(fs + step, nfs)}, device_id_type=MESH)
    pl.semaphore_signal(barrier, inc=1, device_id={"rep": 1 - rep}, device_id_type=MESH)
    for step in range(1, ntp):
        pl.semaphore_signal(barrier, inc=1, device_id={"tp": lax.rem(tp + step, ntp)}, device_id_type=MESH)
    pl.semaphore_wait(barrier, 3 + ntp - 1)

    def region(k, s, half):
        if k < 3 or 4 <= k < first_down:
            index = k if k < 3 else k - 1
            if half is None:
                return rows_w.at[index, at(s, krows), :]
            return rows_w.at[index, at(s * 2 + half, krows // 2), :]
        if k == 3:
            r = slice(None) if half is None else at(half, wo.shape[0] // 2)
            return out_w.at[r, at(s, ocol)]
        r = slice(None) if half is None else at(half, wd.shape[0] // 2)
        return down_w.at[k - first_down, r, at(s, cw)]

    def source(k, half):
        if k < 3:
            ref, c = (wb, wc, wv)[k], slice(None)
        elif k == 3:
            ref, c = wo, slice(None)
        elif k < first_down:
            ref, c = wu, pl.ds((k - 4) * ucol, ucol)
        else:
            ref, c = wd, pl.ds((k - first_down) * cw, cw)
        r = slice(None) if half is None else at(half, ref.shape[0] // 2)
        return ref.at[r, c]

    def hop(k, s, src, sems, to):
        return pltpu.make_async_remote_copy(
            src, region(k, s, rep), sems.at[k, s], recv_z.at[k, s],
            device_id={"fs": to}, device_id_type=MESH)

    def right(k, s, src=None):
        return hop(k, s, region(k, s, rep) if src is None else src, send_r, lax.rem(fs + 1, nfs))

    def left(k, s, src=None):
        return hop(k, s, region(k, s, rep) if src is None else src, send_l, lax.rem(fs + nfs - 1, nfs))

    def across(k, s, half):
        return pltpu.make_async_remote_copy(
            region(k, s, half), region(k, s, half), send_x.at[k, s], recv_x.at[k, s],
            device_id={"rep": 1 - rep}, device_id_type=MESH)

    def send_own(k):
        @pl.when(fs < nfs - 1)
        def _():
            right(k, fs, source(k, rep)).start()

        @pl.when(fs > 0)
        def _():
            left(k, fs, source(k, rep)).start()

    def local(k):
        return pltpu.make_async_copy(source(k, None), region(k, fs, None), local_sem.at[k])

    def advance(k):
        if k + AHEAD < nk:
            send_own(k + AHEAD)

        def one(d, carry):
            @pl.when(fs - d >= 0)
            def _():
                s = fs - d
                right(k, s).wait_recv()

                @pl.when(fs < nfs - 1)
                def _():
                    right(k, s).start()

                across(k, s, rep).start()

            @pl.when(fs + d < nfs)
            def _():
                s = fs + d
                left(k, s).wait_recv()

                @pl.when(fs > 0)
                def _():
                    left(k, s).start()

                across(k, s, rep).start()

            return carry

        lax.fori_loop(1, nfs, one, 0)

    def complete(k):
        def one(s, carry):
            @pl.when(s != fs)
            def _():
                across(k, s, 1 - rep).wait_recv()

            return carry

        lax.fori_loop(0, nfs, one, 0)
        local(k).wait()

    def drain(k):
        def one(s, carry):
            @pl.when((s <= fs) & (fs < nfs - 1))
            def _():
                right(k, s).wait_send()

            @pl.when((s >= fs) & (fs > 0))
            def _():
                left(k, s).wait_send()

            @pl.when(s != fs)
            def _():
                across(k, s, rep).wait_send()

            return carry

        lax.fori_loop(0, nfs, one, 0)

    def group(t, src, dst, send, recv):
        return pltpu.make_async_remote_copy(
            src, dst, send, recv,
            device_id={"tp": lax.rem(tp + t, ntp)}, device_id_type=MESH)

    def tok_copy(t):
        mine = tok.at[:, at(tp, own)]
        return group(t, tokens, mine, tok_send.at[t - 1], tok_recv.at[t - 1])

    def rs_copy(t):
        to = lax.rem(tp + t, ntp)
        return group(t, part.at[:, at(to, own)], rs.at[t - 1], rs_send.at[t - 1], rs_recv.at[t - 1])

    def ag_copy(t):
        mine = mix.at[:, at(tp, own)]
        return group(t, mine, mine, ag_send.at[t - 1], ag_recv.at[t - 1])

    block = nfs * cw
    piece = block // ntp

    def ff_copy(t, c):
        to = lax.rem(tp + t, ntp)
        src = part.at[:, at(c * ntp + to, piece)]
        return group(t, src, rs.at[t - 1, :, pl.ds(c * piece, piece)], ff_send.at[t - 1, c], ff_recv.at[t - 1, c])

    def en_copy(t):
        return group(t, energy.at[0], energy.at[t], en_send.at[t - 1], en_recv.at[t - 1])

    def each_seq(fn):
        def one(i, carry):
            fn(at(i, LEN))
            return carry

        lax.fori_loop(0, seqs, one, 0)

    def factor(v):
        return lax.rsqrt(jnp.mean(v * v, axis=-1, keepdims=True) + epsilon)

    send_own(0)
    for t in range(1, ntp):
        tok_copy(t).start()
    own_tok = pltpu.make_async_copy(tokens, tok.at[:, at(tp, own)], tok_local)
    own_tok.start()
    for k in range(1, AHEAD):
        send_own(k)
    for k in range(nk):
        local(k).start()

    advance(0)
    advance(1)
    own_tok.wait()
    for t in range(1, ntp):
        tok_copy(t).wait_recv()

    def norm_tokens(r):
        v = tok[r, :].astype(F32)
        normed[r, :] = (v * factor(v) * gain1[...].astype(F32)).astype(BF16)

    each_seq(norm_tokens)
    advance(2)
    advance(3)
    for k in range(3):
        complete(k)

    own_taps = taps[:, at(tp, chan)].astype(F32)
    position = lax.broadcasted_iota(jnp.int32, (LEN, chan), 0)

    def mixer(r):
        rows = normed[r, :]
        inner = dot(rows, rows_w[1]).astype(BF16).astype(F32) * dot(rows, rows_w[2]).astype(BF16).astype(F32)
        before = jnp.where(position == 0, 0.0, pltpu.roll(inner, 1, 0))
        after = jnp.where(position == LEN - 1, 0.0, pltpu.roll(inner, LEN - 1, 0))
        conv = own_taps[0:1] * before + own_taps[1:2] * inner + own_taps[2:3] * after
        outer = dot(rows, rows_w[0]).astype(BF16).astype(F32)
        active[r, 0:chan] = (outer * conv).astype(BF16)

    each_seq(mixer)
    advance(4)
    complete(3)

    def project(r):
        part[r, :] = dot(active[r, 0:chan], out_w[...]).astype(BF16)

    each_seq(project)
    for t in range(1, ntp):
        rs_copy(t).start()
    done = 5
    for k in range(done, min(first_down, nk)):
        advance(k)
    for t in range(1, ntp):
        rs_copy(t).wait_recv()

    def add_mix(r):
        total = part[r, at(tp, own)].astype(F32)
        for t in range(1, ntp):
            total = total + rs[t - 1, r, :].astype(F32)
        mix[r, at(tp, own)] = total.astype(BF16)

    each_seq(add_mix)
    for t in range(1, ntp):
        ag_copy(t).start()
    early = max(nc - 2, 0)
    for c in range(early):
        advance(first_down + c)
    for k in range(4, first_down):
        complete(k)
    for t in range(1, ntp):
        ag_copy(t).wait_recv()

    def second(r):
        m = mix[r, :].astype(F32)
        res = (tok[r, :].astype(F32) + m * factor(m) * gain2[...].astype(F32)).astype(BF16)
        tok[r, :] = res
        res = res.astype(F32)
        rows = (res * factor(res) * gain3[...].astype(F32)).astype(BF16)
        for u in range(nu):
            lifted = jnp.maximum(dot(rows, rows_w[3 + u]), 0.0)
            active[r, pl.ds(u * ucol, ucol)] = (lifted * lifted).astype(BF16)

    for t in range(1, ntp):
        tok_copy(t).wait_send()
        rs_copy(t).wait_send()
    each_seq(second)

    for c in range(nc):
        if early <= c + 1 < nc:
            advance(first_down + c + 1)
        if c == 0 and early == 0:
            advance(first_down)
        complete(first_down + c)

        def down(r):
            part[r, pl.ds(c * block, block)] = dot(active[r, :], down_w[c]).astype(BF16)

        each_seq(down)
        for t in range(1, ntp):
            ff_copy(t, c).start()

    for k in range(nk):
        drain(k)
    for t in range(1, ntp):
        ag_copy(t).wait_send()
        for c in range(nc):
            ff_copy(t, c).wait_recv()

    def own_ffn(r):
        pieces = [part[r, at(c * ntp + tp, piece)] for c in range(nc)]
        total = (pieces[0] if nc == 1 else jnp.concatenate(pieces, axis=1)).astype(F32)
        for t in range(1, ntp):
            total = total + rs[t - 1, r, :].astype(F32)
        return total

    def measure(r):
        total = own_ffn(r)
        square = jnp.sum(total * total, axis=1, keepdims=True)
        flat = jnp.transpose(jnp.broadcast_to(square, (LEN, LANES)))
        energy[0, :, r] = flat[0:8, :]

    each_seq(measure)
    for t in range(1, ntp):
        en_copy(t).start()
    for t in range(1, ntp):
        en_copy(t).wait_recv()
    own_gain = gain4[:, at(tp, own)].astype(F32)

    def close(r):
        total = own_ffn(r)
        flat = energy[0, :, r]
        for t in range(1, ntp):
            flat = flat + energy[t, :, r]
        tall = jnp.transpose(jnp.concatenate([flat] * (LANES // 8), axis=0))
        scale = lax.rsqrt(tall[:, 0:1] / width + epsilon)
        result[r, :] = (tok[r, at(tp, own)].astype(F32) + total * scale * own_gain).astype(BF16)

    each_seq(close)
    for t in range(1, ntp):
        en_copy(t).wait_send()
        for c in range(nc):
            ff_copy(t, c).wait_send()


def solution(mesh):
    nfs, ntp = mesh.shape["fs"], mesh.shape["tp"]
    assert mesh.shape["rep"] == 2

    def body(tokens, gain1, wb, wc, wv, taps, wo, gain2, gain3, wu, wd, gain4):
        count, own = tokens.shape
        width, chan, hidden = own * ntp, wb.shape[1], wu.shape[1]
        ucol = chan
        nu = hidden // ucol
        cw = min(LANES, wd.shape[1])
        nc = wd.shape[1] // cw
        nk = 4 + nu + nc
        vm, anyw = pl.BlockSpec(memory_space=pltpu.VMEM), pl.BlockSpec(memory_space=pl.ANY)
        dma = pltpu.SemaphoreType.DMA
        peers = ntp - 1
        return pl.pallas_call(
            functools.partial(kernel, nfs, ntp, nu, nc, cw),
            out_shape=jax.ShapeDtypeStruct((count, own), BF16),
            in_specs=[anyw, vm, anyw, anyw, anyw, vm, anyw, vm, vm, anyw, anyw, vm],
            out_specs=vm,
            scratch_shapes=[
                pltpu.VMEM((3 + nu, width, chan), BF16),
                pltpu.VMEM((chan, width), BF16),
                pltpu.VMEM((nc, hidden, nfs * cw), BF16),
                pltpu.VMEM((count, width), BF16),
                pltpu.VMEM((count, width), BF16),
                pltpu.VMEM((count, width), BF16),
                pltpu.VMEM((peers, count, own), BF16),
                pltpu.VMEM((count, width), BF16),
                pltpu.VMEM((count, hidden), BF16),
                pltpu.VMEM((ntp, 8, count), F32),
                dma((nk, nfs)), dma((nk, nfs)), dma((nk, nfs)), dma((nk, nfs)), dma((nk, nfs)),
                dma((nk,)), dma,
                dma((peers,)), dma((peers,)), dma((peers,)), dma((peers,)),
                dma((peers,)), dma((peers,)), dma((peers, nc)), dma((peers, nc)),
                dma((peers,)), dma((peers,)),
            ],
            compiler_params=pltpu.CompilerParams(
                collective_id=0, has_side_effects=True, vmem_limit_bytes=64000000),
            name="layer",
        )(tokens, gain1[None], wb, wc, wv, taps, wo, gain2[None], gain3[None], wu, wd, gain4[None])

    placed = (
        P(("rep", "fs"), "tp"), P(), P("fs", "tp"), P("fs", "tp"), P("fs", "tp"), P(), P("tp", "fs"),
        P(), P(), P("fs", "tp"), P("tp", "fs"), P(),
    )
    return jax.shard_map(
        body, mesh=mesh, in_specs=placed, out_specs=P(("rep", "fs"), "tp"), check_vma=False
    )
```
